256 devices in a mesh: grp: 2 (over y), sp: 32 (over z, core), tp: 4 (over x).
Axes of the slice: x: 4, y: 2, z: 16, core: 2. Of those that a mesh axis runs over, the one named last changes fastest.
The devices are a block of a 4x16x16 slice.
Arguments:
- resid: bfloat16 [40960, 2048], P(('grp', 'sp'), 'tp'), parts along dimension 0, may hold values from -6 to 6
- queries: bfloat16 [40960, 2048], P(('grp', 'sp'), 'tp'), parts along dimension 0, may hold values from -150 to 150
- keys_values: bfloat16 [40960, 8, 128], P(('grp', 'sp'), 'tp'), parts along dimension 0, may hold values from -4.5 to 4.5
- sink: float32 [32], P('tp'), may hold values from 3 to 7
- out_weight: bfloat16 [2048, 2048], P('tp'), may hold values from -2.390625 to 2.390625
- norm_gain: float32 [2048], replicated, may hold values from 0.1 to 1.9
- gate_weight: bfloat16 [2048, 5632], P('sp', 'tp'), may hold values from -0.125 to 0.125
- up_weight: bfloat16 [2048, 5632], P('sp', 'tp'), may hold values from -0.125 to 0.125
- down_weight: bfloat16 [5632, 2048], P('tp', 'sp'), may hold values from -0.078125 to 0.078125
Outputs:
- mixed: bfloat16 [40960, 2048], P(('grp', 'sp'), 'tp'), parts along dimension 0
The draws below stay inside these ranges and needn't reach their ends.
There are 2 independent parts, one for each index of `grp`. The reference program is written for one: setup_inputs(seed, part) draws one part's arguments, and reference() takes and returns one part's arrays. A program takes and returns all parts, laid end to end along the dimension named above; an argument that names none is the same for every part. Nothing has to cross between parts.
All inputs are finite; a program needn't handle non-finite values.
Results may differ from the reference program's by a relative error of at most 0.008.
Values may be sent and summed in bfloat16 or wider, within the bound.
No kernel may reach another device: no remote copies, remote signals or barrier semaphores. Data moves between devices by JAX's collectives and lax.ppermute only.
A program may use at most 128 MiB of HBM per device.

```python
import jax
import jax.numpy as jnp
from jax import lax

D = 2048
HEADS = 32
KV_HEADS = 8
HEAD_DIM = 64
FF = 5632
WINDOW = 128
GRID_W = 64
TOKENS = 20480


def joint_draw(key):
    both = jnp.clip(jax.random.normal(jax.random.fold_in(key, 11), (TOKENS, KV_HEADS, 2 * HEAD_DIM), jnp.float32), -4.5, 4.5)
    drawn = jnp.clip(jax.random.normal(jax.random.fold_in(key, 12), (TOKENS, HEADS * HEAD_DIM), jnp.float32), -4.5, 4.5)
    return (drawn, both)


def draw_queries(key, part):
    drawn, both = joint_draw(key)
    return drawn.astype(jnp.bfloat16)


def draw_keys_values(key, part):
    drawn, both = joint_draw(key)
    return both.astype(jnp.bfloat16)


def shard_levels(rng, extent, split, smallest, largest):
    gain, own = 1.0, jax.random.fold_in(rng, 6)
    for dim, blocks in split:
        steps = jnp.exp(jax.random.uniform(jax.random.fold_in(own, dim), (blocks,), jnp.float32, smallest / len(split), largest / len(split)))
        gain = gain * jnp.repeat(steps, extent[dim] // blocks).reshape([-1 if axis == dim else 1 for axis in range(len(extent))])
    return gain


def normal_values(key, dims, deviation, most, split=(), held_as=jnp.bfloat16):
    entries = jax.random.normal(key, dims, jnp.float32) * deviation
    if len(split) > 0:
        entries = shard_levels(key, dims, split, -0.22, 0.18) * entries
    return jnp.clip(entries, min=-most, max=most).astype(held_as)


def setup_inputs(seed: int = 0, part: int = 0) -> dict:
    streams_of = jax.random.split(jax.random.key(seed), 10)
    part_keys = jax.random.split(jax.random.fold_in(streams_of[9], part), 10)
    return {
        "resid": normal_values(part_keys[0], (TOKENS, D), 1.0, 6.0, ((0, 32), (1, 4))),
        "queries": draw_queries(jax.random.fold_in(jax.random.fold_in(streams_of[9], part), 71), part),
        "keys_values": draw_keys_values(jax.random.fold_in(jax.random.fold_in(streams_of[9], part), 71), part),
        "sink": jnp.clip(3.0 + 4.0 * jax.random.uniform(streams_of[3], (HEADS,), jnp.float32) ** shard_levels(streams_of[3], (HEADS,), ((0, 4),), -0.2, 0.2), 3.0, 7.0),
        "out_weight": normal_values(streams_of[4], (HEADS * HEAD_DIM, D), 0.4, 2.390625, ((0, 4),)),
        "norm_gain": jnp.clip(1.0 + 0.18 * jax.random.normal(streams_of[5], (D,), jnp.float32), 0.1, 1.9),
        "gate_weight": normal_values(streams_of[6], (D, FF), D ** -0.5, 0.125, ((0, 32), (1, 4))),
        "up_weight": normal_values(streams_of[7], (D, FF), D ** -0.5, 0.125, ((0, 32), (1, 4))),
        "down_weight": normal_values(streams_of[8], (FF, D), FF ** -0.5, 0.078125, ((0, 4), (1, 32))),
    }


def rotate(values, positions):
    quarter = 16
    inverse = 10000.0 ** (-jnp.arange(quarter, dtype=jnp.float32) / quarter)

    def turn(part, place):
        angle = place.astype(jnp.float32)[:, None] * inverse[None, :]
        cosine = jnp.cos(angle)[:, None, :]
        sine = jnp.sin(angle)[:, None, :]
        first, second = (part[..., :quarter], part[..., quarter:])
        return jnp.concatenate([first * cosine - second * sine, second * cosine + first * sine], axis=-1)
    grid_row = positions // GRID_W
    grid_col = positions % GRID_W
    return jnp.concatenate([turn(values[..., :32], grid_row), turn(values[..., 32:], grid_col)], axis=-1)

def reference(resid, queries, keys_values, sink, out_weight, norm_gain, gate_weight, up_weight, down_weight):
    group = HEADS // KV_HEADS
    positions = jnp.arange(TOKENS, dtype=jnp.int32)
    rotated_q = rotate(queries.astype(jnp.float32).reshape(TOKENS, HEADS, HEAD_DIM), positions).astype(jnp.bfloat16)
    rotated_k = rotate(keys_values[..., :HEAD_DIM].astype(jnp.float32), positions).astype(jnp.bfloat16)
    padded_k = jnp.pad(rotated_k, ((WINDOW, WINDOW), (0, 0), (0, 0)))
    padded_v = jnp.pad(keys_values[..., HEAD_DIM:], ((WINDOW, WINDOW), (0, 0), (0, 0)))
    sink_grid = sink.reshape(KV_HEADS, group)[:, :, None]

    def block(index):
        start = (index * WINDOW).astype(jnp.int32)
        zero = jnp.int32(0)
        query_block = lax.dynamic_slice(rotated_q, (start, zero, zero), (WINDOW, HEADS, HEAD_DIM))
        key_block = lax.dynamic_slice(padded_k, (start, zero, zero), (3 * WINDOW, KV_HEADS, HEAD_DIM))
        value_block = lax.dynamic_slice(padded_v, (start, zero, zero), (3 * WINDOW, KV_HEADS, HEAD_DIM))
        grouped = query_block.astype(jnp.float32).reshape(WINDOW, KV_HEADS, group, HEAD_DIM)
        scores = jnp.einsum('qkgd,jkd->kgqj', grouped, key_block.astype(jnp.float32)) * HEAD_DIM ** (-0.5)
        query_pos = start + jnp.arange(WINDOW, dtype=jnp.int32)
        key_pos = start - WINDOW + jnp.arange(3 * WINDOW, dtype=jnp.int32)
        valid = (jnp.abs(query_pos[:, None] - key_pos[None, :]) <= WINDOW) & (key_pos[None, :] >= 0) & (key_pos[None, :] < TOKENS)
        scores = jnp.where(valid[None, None], scores, jnp.float32(-1e+30))
        top = jnp.maximum(lax.optimization_barrier(jnp.max(scores, axis=-1)), sink_grid)
        expo = jnp.exp(scores - top[..., None])
        total = lax.optimization_barrier(jnp.sum(expo, axis=-1)) + jnp.exp(sink_grid - top)
        probs = (expo / total[..., None]).astype(jnp.bfloat16)
        result = jnp.einsum('kgqj,jkd->qkgd', probs.astype(jnp.float32), value_block.astype(jnp.float32))
        return result.astype(jnp.bfloat16).reshape(WINDOW, HEADS * HEAD_DIM)
    attended = lax.map(block, jnp.arange(TOKENS // WINDOW, dtype=jnp.int32)).reshape(TOKENS, HEADS * HEAD_DIM)
    stream = (resid.astype(jnp.float32) + jnp.dot(attended, out_weight, preferred_element_type=jnp.float32)).astype(jnp.bfloat16)
    widened = stream.astype(jnp.float32)
    normed = (widened * lax.rsqrt(lax.optimization_barrier(jnp.mean(widened * widened, axis=-1, keepdims=True)) + 1e-06) * norm_gain).astype(jnp.bfloat16)
    gate = jnp.dot(normed, gate_weight, preferred_element_type=jnp.float32)
    up = jnp.dot(normed, up_weight, preferred_element_type=jnp.float32)
    hidden = (jax.nn.silu(gate) * up).astype(jnp.bfloat16)
    return (stream.astype(jnp.float32) + jnp.dot(hidden, down_weight, preferred_element_type=jnp.float32)).astype(jnp.bfloat16)
```

```python
import jax
import jax.numpy as jnp
from jax import lax
from jax.sharding import PartitionSpec as P

HEAD_DIM = 64
WINDOW = 128
GRID_W = 64


def with_halo(cells, sides, width):
    for axis, dim in sides:
        count = lax.axis_size(axis)
        ends = count - 1
        head = lax.slice_in_dim(cells, 0, width, axis=dim)
        tail = lax.slice_in_dim(cells, cells.shape[dim] - width, cells.shape[dim], axis=dim)
        cells = jnp.concatenate(
            [
                lax.ppermute(tail, axis, [(i, (i + 1) % count) for i in range(ends)]),
                cells,
                lax.ppermute(head, axis, [((i + 1) % count, i) for i in range(ends)]),
            ],
            axis=dim,
        )
    return cells


def cut_along(array, dim, devices):
    before, after = (array.shape[:dim], array.shape[dim + 1 :])
    return jnp.moveaxis(array.reshape(*before, devices, -1, *after), dim, 0)


def sum_at_owner(array, axis, dim):
    blocks = cut_along(array, dim, lax.axis_size(axis))
    arrived = lax.all_to_all(blocks, axis, split_axis=0, concat_axis=0, tiled=True)
    return arrived.sum(axis=0)


def in_order(blocks, dim):
    shape = list(blocks.shape[1:])
    shape[dim] *= blocks.shape[0]
    return jnp.moveaxis(blocks, 0, dim).reshape(shape)


def copy_for_each(array, axis):
    copies = jnp.broadcast_to(array, (lax.axis_size(axis), *array.shape))
    return lax.all_to_all(copies, axis, split_axis=0, concat_axis=0, tiled=True)


def collect(array, axis, dim):
    return in_order(copy_for_each(array, axis), dim)


def side_by_side(arrays, axis, dim, along):
    both = jnp.concatenate(arrays, axis=along)
    out, at, done = (lax.all_gather(both, axis, axis=dim, tiled=True), 0, [])
    for a in arrays:
        done.append(lax.slice_in_dim(out, at, at + a.shape[along], axis=along))
        at += a.shape[along]
    return tuple(done)


def summed_on_arrival(array, axis, dim):
    blocks = cut_along(array, dim, lax.axis_size(axis))
    arrived = lax.all_to_all(blocks, axis, split_axis=0, concat_axis=0, tiled=True)
    return arrived.astype(jnp.float32).sum(axis=0)


def rotate(values, positions):
    quarter = 16
    inverse = 10000.0 ** (-jnp.arange(quarter, dtype=jnp.float32) / quarter)

    def turn(part, place):
        angle = place.astype(jnp.float32)[:, None] * inverse[None, :]
        cosine = jnp.cos(angle)[:, None, :]
        sine = jnp.sin(angle)[:, None, :]
        first, second = (part[..., :quarter], part[..., quarter:])
        return jnp.concatenate(
            [first * cosine - second * sine, second * cosine + first * sine], axis=-1
        )

    grid_row = positions // GRID_W
    grid_col = positions % GRID_W
    return jnp.concatenate(
        [turn(values[..., :32], grid_row), turn(values[..., 32:], grid_col)], axis=-1
    )


def body(
    resid, queries, keys_values, sink, out_weight, norm_gain, gate_weight, up_weight, down_weight
):
    tok = queries.shape[0]
    heads_here = queries.shape[1] // HEAD_DIM
    kv_here = keys_values.shape[1]
    group = heads_here // kv_here
    offset = lax.axis_index("sp") * tok
    total_tokens = tok * lax.axis_size("sp")
    positions = offset + jnp.arange(tok, dtype=jnp.int32)
    rotated_q = rotate(
        queries.astype(jnp.float32).reshape(tok, heads_here, HEAD_DIM), positions
    ).astype(jnp.bfloat16)
    rotated_k = rotate(keys_values[..., :HEAD_DIM].astype(jnp.float32), positions).astype(
        jnp.bfloat16
    )
    joined = jnp.concatenate([rotated_k, keys_values[..., HEAD_DIM:]], axis=-1)
    padded = with_halo(joined, (("sp", 0),), WINDOW)
    blocks = tok // WINDOW
    key_blocks = jnp.stack(
        [padded[index * WINDOW : index * WINDOW + 3 * WINDOW] for index in range(blocks)]
    )
    grouped = rotated_q.reshape(blocks, WINDOW, kv_here, group, HEAD_DIM)
    scores = jnp.einsum(
        "nqkgd,njkd->nkgqj", grouped, key_blocks[..., :HEAD_DIM], preferred_element_type=jnp.float32
    ) * HEAD_DIM ** (-0.5)
    block_start = offset + WINDOW * jnp.arange(blocks, dtype=jnp.int32)
    query_pos = block_start[:, None] + jnp.arange(WINDOW, dtype=jnp.int32)[None, :]
    key_pos = block_start[:, None] - WINDOW + jnp.arange(3 * WINDOW, dtype=jnp.int32)[None, :]
    valid = (
        (jnp.abs(query_pos[:, :, None] - key_pos[:, None, :]) <= WINDOW)
        & (key_pos[:, None, :] >= 0)
        & (key_pos[:, None, :] < total_tokens)
    )
    scores = jnp.where(valid[:, None, None], scores, jnp.float32(-1e30))
    sink_grid = sink.reshape(kv_here, group)[None, :, :, None]
    top = jnp.maximum(jnp.max(scores, axis=-1), sink_grid)
    expo = jnp.exp(scores - top[..., None])
    denom = jnp.sum(expo, axis=-1) + jnp.exp(sink_grid - top)
    probs = (expo / denom[..., None]).astype(jnp.bfloat16)
    attended = jnp.einsum(
        "nkgqj,njkd->nqkgd", probs, key_blocks[..., HEAD_DIM:], preferred_element_type=jnp.float32
    )
    attended = attended.astype(jnp.bfloat16).reshape(tok, heads_here * HEAD_DIM)
    partial_proj = jnp.dot(attended, out_weight, preferred_element_type=jnp.float32)
    projected = summed_on_arrival(partial_proj.astype(jnp.bfloat16), "tp", 1)
    stream_cols = (resid.astype(jnp.float32) + projected).astype(jnp.bfloat16)
    stream = collect(stream_cols, "tp", 1)
    widened = stream.astype(jnp.float32)
    normed = (
        widened * lax.rsqrt(jnp.mean(widened * widened, axis=-1, keepdims=True) + 1e-06) * norm_gain
    ).astype(jnp.bfloat16)
    pieces = side_by_side((gate_weight, up_weight, down_weight.T), "sp", 0, 1)
    gate = jnp.dot(normed, pieces[0], preferred_element_type=jnp.float32)
    up = jnp.dot(normed, pieces[1], preferred_element_type=jnp.float32)
    hidden = lax.optimization_barrier((jax.nn.silu(gate) * up).astype(jnp.bfloat16))
    terms = lax.dot_general(
        hidden, pieces[2], (((1,), (1,)), ((), ())), preferred_element_type=jnp.float32
    )
    summed = summed_on_arrival(terms.astype(jnp.bfloat16), "tp", 1)
    return (stream_cols.astype(jnp.float32) + summed).astype(jnp.bfloat16)


def solution(mesh):
    return jax.shard_map(
        body,
        mesh=mesh,
        in_specs=(
            P(("grp", "sp"), "tp"),
            P(("grp", "sp"), "tp"),
            P(("grp", "sp"), "tp", None),
            P("tp"),
            P("tp", None),
            P(),
            P("sp", "tp"),
            P("sp", "tp"),
            P("tp", "sp"),
        ),
        out_specs=P(("grp", "sp"), "tp"),
        check_vma=False,
    )
```

```python
import jax
import jax.numpy as jnp
from jax import lax
from jax.experimental import pallas as pl
from jax.experimental.pallas import tpu as pltpu
from jax.sharding import PartitionSpec as P


HEAD_DIM = 64
WINDOW = 128
GRID_W = 64


def with_halo(cells, sides, width):
    for axis, dim in sides:
        count = lax.axis_size(axis)
        ends = count - 1
        head = lax.slice_in_dim(cells, 0, width, axis=dim)
        tail = lax.slice_in_dim(cells, cells.shape[dim] - width, cells.shape[dim], axis=dim)
        cells = jnp.concatenate(
            [
                lax.ppermute(tail, axis, [(i, (i + 1) % count) for i in range(ends)]),
                cells,
                lax.ppermute(head, axis, [((i + 1) % count, i) for i in range(ends)]),
            ],
            axis=dim,
        )
    return cells


def cut_along(array, dim, devices):
    before, after = (array.shape[:dim], array.shape[dim + 1 :])
    return jnp.moveaxis(array.reshape(*before, devices, -1, *after), dim, 0)


def sum_at_owner(array, axis, dim):
    blocks = cut_along(array, dim, lax.axis_size(axis))
    arrived = lax.all_to_all(blocks, axis, split_axis=0, concat_axis=0, tiled=True)
    return arrived.sum(axis=0)


def in_order(blocks, dim):
    shape = list(blocks.shape[1:])
    shape[dim] *= blocks.shape[0]
    return jnp.moveaxis(blocks, 0, dim).reshape(shape)


def copy_for_each(array, axis):
    copies = jnp.broadcast_to(array, (lax.axis_size(axis), *array.shape))
    return lax.all_to_all(copies, axis, split_axis=0, concat_axis=0, tiled=True)


def collect(array, axis, dim):
    return in_order(copy_for_each(array, axis), dim)


def summed_on_arrival(array, axis, dim):
    blocks = cut_along(array, dim, lax.axis_size(axis))
    arrived = lax.all_to_all(blocks, axis, split_axis=0, concat_axis=0, tiled=True)
    return arrived.astype(jnp.float32).sum(axis=0)


def gated_kernel(normed_ref, gate_ref, up_ref, hidden_ref):
    width = gate_ref.shape[1]
    both = jnp.concatenate([gate_ref[...], up_ref[...]], axis=1)
    product = jnp.dot(normed_ref[...], both, preferred_element_type=jnp.float32)
    gate = product[:, :width]
    up = product[:, width:]
    hidden_ref[...] = (gate / (1.0 + jnp.exp(-gate)) * up).astype(jnp.bfloat16)


def gated(normed, weights, hidden_units):
    tok, model = normed.shape
    width = 128
    steps = hidden_units // width
    return pl.pallas_call(
        gated_kernel,
        grid=(steps,),
        in_specs=[
            pl.BlockSpec((tok, model), lambda j: (0, 0)),
            pl.BlockSpec((model, width), lambda j: (0, j)),
            pl.BlockSpec((model, width), lambda j: (0, j + steps)),
        ],
        out_specs=pl.BlockSpec((tok, width), lambda j: (0, j)),
        out_shape=jax.ShapeDtypeStruct((tok, hidden_units), jnp.bfloat16),
        cost_estimate=pl.CostEstimate(
            flops=4 * tok * model * hidden_units,
            bytes_accessed=4 * model * hidden_units + 2 * tok * (model + hidden_units),
            transcendentals=tok * hidden_units,
        ),
        name="gated",
    )(normed, weights, weights)


def share_kernel(owner_ref, hidden_ref, down_ref, first_ref, second_ref):
    half = first_ref.shape[0]
    terms = lax.dot_general(
        hidden_ref[...],
        down_ref[...],
        (((1,), (1,)), ((), ())),
        preferred_element_type=jnp.float32,
    )
    first_ref[...] = terms[:half].astype(first_ref.dtype)
    second_ref[...] = terms[half:].astype(second_ref.dtype)


def share(hidden, weights, owner, width, dtype):
    tok, units = hidden.shape
    half = tok // 2
    out = jax.ShapeDtypeStruct((half, width), dtype)
    return pl.pallas_call(
        share_kernel,
        grid_spec=pltpu.PrefetchScalarGridSpec(
            num_scalar_prefetch=1,
            grid=(1,),
            in_specs=[
                pl.BlockSpec((tok, units), lambda j, o: (0, 0)),
                pl.BlockSpec((width, units), lambda j, o: (o[0], 2)),
            ],
            out_specs=[
                pl.BlockSpec((half, width), lambda j, o: (0, 0)),
                pl.BlockSpec((half, width), lambda j, o: (0, 0)),
            ],
        ),
        out_shape=[out, out],
        cost_estimate=pl.CostEstimate(
            flops=2 * tok * units * width,
            bytes_accessed=2 * units * (tok + width) + 2 * tok * width,
            transcendentals=0,
        ),
        name="share",
    )(owner.reshape(1), hidden, weights)


def shifted(array, axis, by):
    count = lax.axis_size(axis)
    return lax.ppermute(array, axis, [(i, (i + by) % count) for i in range(count)])


def added(*terms):
    return sum((t.astype(jnp.float32) for t in terms[1:]), terms[0].astype(jnp.float32))


def down_at_owner(hidden, weights, axis):
    count = lax.axis_size(axis)
    width = weights.shape[0] // count
    me = lax.axis_index(axis)
    far_top, far_low = share(hidden, weights, (me + 2) % count, width, jnp.bfloat16)
    far_top_in = shifted(far_top, axis, 1)
    far_low_in = shifted(far_low, axis, -1)
    right_top, right_low = share(hidden, weights, (me + 1) % count, width, jnp.bfloat16)
    left_top, left_low = share(hidden, weights, (me + count - 1) % count, width, jnp.bfloat16)
    right_low_in = shifted(right_low, axis, 1)
    left_top_in = shifted(left_top, axis, -1)
    own_top, own_low = share(hidden, weights, me, width, jnp.float32)
    relay_right = added(right_top, far_top_in).astype(jnp.bfloat16)
    relay_left = added(left_low, far_low_in).astype(jnp.bfloat16)
    relay_top_in = shifted(relay_right, axis, 1)
    relay_low_in = shifted(relay_left, axis, -1)
    return (added(own_top, left_top_in, relay_top_in), added(own_low, right_low_in, relay_low_in))


def rotate(values, positions):
    quarter = 16
    inverse = 10000.0 ** (-jnp.arange(quarter, dtype=jnp.float32) / quarter)

    def turn(part, place):
        angle = place.astype(jnp.float32)[:, None] * inverse[None, :]
        cosine = jnp.cos(angle)[:, None, :]
        sine = jnp.sin(angle)[:, None, :]
        first, second = (part[..., :quarter], part[..., quarter:])
        return jnp.concatenate(
            [first * cosine - second * sine, second * cosine + first * sine], axis=-1
        )

    grid_row = positions // GRID_W
    grid_col = positions % GRID_W
    return jnp.concatenate(
        [turn(values[..., :32], grid_row), turn(values[..., 32:], grid_col)], axis=-1
    )


def body(
    resid, queries, keys_values, sink, out_weight, norm_gain, gate_weight, up_weight, down_weight
):
    tok = queries.shape[0]
    heads_here = queries.shape[1] // HEAD_DIM
    kv_here = keys_values.shape[1]
    group = heads_here // kv_here
    offset = lax.axis_index("sp") * tok
    total_tokens = tok * lax.axis_size("sp")
    positions = offset + jnp.arange(tok, dtype=jnp.int32)
    rotated_q = rotate(
        queries.astype(jnp.float32).reshape(tok, heads_here, HEAD_DIM), positions
    ).astype(jnp.bfloat16)
    rotated_k = rotate(keys_values[..., :HEAD_DIM].astype(jnp.float32), positions).astype(
        jnp.bfloat16
    )
    joined = jnp.concatenate([rotated_k, keys_values[..., HEAD_DIM:]], axis=-1)
    padded = with_halo(joined, (("sp", 0),), WINDOW)
    blocks = tok // WINDOW
    key_blocks = jnp.stack(
        [padded[index * WINDOW : index * WINDOW + 3 * WINDOW] for index in range(blocks)]
    )
    grouped = rotated_q.reshape(blocks, WINDOW, kv_here, group, HEAD_DIM)
    scores = jnp.einsum(
        "nqkgd,njkd->nkgqj", grouped, key_blocks[..., :HEAD_DIM], preferred_element_type=jnp.float32
    ) * HEAD_DIM ** (-0.5)
    block_start = offset + WINDOW * jnp.arange(blocks, dtype=jnp.int32)
    query_pos = block_start[:, None] + jnp.arange(WINDOW, dtype=jnp.int32)[None, :]
    key_pos = block_start[:, None] - WINDOW + jnp.arange(3 * WINDOW, dtype=jnp.int32)[None, :]
    valid = (
        (jnp.abs(query_pos[:, :, None] - key_pos[:, None, :]) <= WINDOW)
        & (key_pos[:, None, :] >= 0)
        & (key_pos[:, None, :] < total_tokens)
    )
    scores = jnp.where(valid[:, None, None], scores, jnp.float32(-1e30))
    sink_grid = sink.reshape(kv_here, group)[None, :, :, None]
    top = jnp.maximum(jnp.max(scores, axis=-1), sink_grid)
    expo = jnp.exp(scores - top[..., None])
    denom = jnp.sum(expo, axis=-1) + jnp.exp(sink_grid - top)
    probs = (expo / denom[..., None]).astype(jnp.bfloat16)
    attended = jnp.einsum(
        "nkgqj,njkd->nqkgd", probs, key_blocks[..., HEAD_DIM:], preferred_element_type=jnp.float32
    )
    attended = attended.astype(jnp.bfloat16).reshape(tok, heads_here * HEAD_DIM)
    partial_proj = jnp.dot(attended, out_weight, preferred_element_type=jnp.float32)
    projected = summed_on_arrival(partial_proj.astype(jnp.bfloat16), "tp", 1)
    stream_cols = (resid.astype(jnp.float32) + projected).astype(jnp.bfloat16)
    stream = collect(stream_cols, "tp", 1)
    widened = stream.astype(jnp.float32)
    normed = (
        widened * lax.rsqrt(jnp.mean(widened * widened, axis=-1, keepdims=True) + 1e-06) * norm_gain
    ).astype(jnp.bfloat16)
    hidden_units = gate_weight.shape[1]
    shard = jnp.concatenate((gate_weight, up_weight, down_weight.T), axis=1)
    weights = lax.all_gather(shard, "sp", axis=0, tiled=True)
    hidden = gated(normed, weights, hidden_units)
    summed = jnp.concatenate(down_at_owner(hidden, weights, "tp"), axis=0)
    return (stream_cols.astype(jnp.float32) + summed).astype(jnp.bfloat16)


def solution(mesh):
    return jax.shard_map(
        body,
        mesh=mesh,
        in_specs=(
            P(("grp", "sp"), "tp"),
            P(("grp", "sp"), "tp"),
            P(("grp", "sp"), "tp", None),
            P("tp"),
            P("tp", None),
            P(),
            P("sp", "tp"),
            P("sp", "tp"),
            P("tp", "sp"),
        ),
        out_specs=P(("grp", "sp"), "tp"),
        check_vma=False,
    )
```

```python
import jax
import jax.numpy as jnp
from jax import lax
from jax.experimental import pallas as pl
from jax.experimental.pallas import tpu as pltpu
from jax.sharding import PartitionSpec as P


HEAD_DIM = 64
WINDOW = 128
GRID_W = 64


def with_halo(cells, sides, width):
    for axis, dim in sides:
        count = lax.axis_size(axis)
        ends = count - 1
        head = lax.slice_in_dim(cells, 0, width, axis=dim)
        tail = lax.slice_in_dim(cells, cells.shape[dim] - width, cells.shape[dim], axis=dim)
        cells = jnp.concatenate(
            [
                lax.ppermute(tail, axis, [(i, (i + 1) % count) for i in range(ends)]),
                cells,
                lax.ppermute(head, axis, [((i + 1) % count, i) for i in range(ends)]),
            ],
            axis=dim,
        )
    return cells


def shifted(array, axis, by):
    count = lax.axis_size(axis)
    return lax.ppermute(array, axis, [(i, (i + by) % count) for i in range(count)])


def added(*terms):
    return sum((t.astype(jnp.float32) for t in terms[1:]), terms[0].astype(jnp.float32))


def settle_kernel(own_ref, top_ref, top2_ref, low_ref, low2_ref, out_ref):
    half = top_ref.shape[0]
    out_ref[:half] = added(own_ref[:half], top_ref[...], top2_ref[...]).astype(out_ref.dtype)
    out_ref[half:] = added(own_ref[half:], low_ref[...], low2_ref[...]).astype(out_ref.dtype)


def settle(own, tops, lows):
    vmem = pl.BlockSpec(memory_space=pltpu.VMEM)
    return pl.pallas_call(
        settle_kernel,
        in_specs=[vmem] * 5,
        out_specs=vmem,
        out_shape=jax.ShapeDtypeStruct(own.shape, jnp.bfloat16),
        cost_estimate=pl.CostEstimate(
            flops=2 * own.size, bytes_accessed=10 * own.size, transcendentals=0
        ),
        compiler_params=pltpu.CompilerParams(vmem_limit_bytes=12 << 20),
        name="settle",
    )(own, *tops, *lows)


def relayed(far_in, mine):
    return added(mine, far_in).astype(jnp.bfloat16)


def ring_places(axis):
    count = lax.axis_size(axis)
    me = lax.axis_index(axis)
    return jnp.stack([(me + by) % count for by in (2, 1, count - 1, 0)]).astype(jnp.int32)


def ring_sum(far, right, left, own, axis):
    far_top_in = shifted(far[0], axis, 1)
    far_low_in = shifted(far[1], axis, -1)
    right_low_in = shifted(right[1], axis, 1)
    left_top_in = shifted(left[0], axis, -1)
    relay_top_in = shifted(relayed(far_top_in, right[0]), axis, 1)
    relay_low_in = shifted(relayed(far_low_in, left[1]), axis, -1)
    return settle(own, (left_top_in, relay_top_in), (right_low_in, relay_low_in))


def project_kernel(places_ref, rows_ref, weight_ref, base_ref, *outs):
    half = outs[0].shape[0]
    step = pl.program_id(0)
    terms = jnp.dot(rows_ref[...], weight_ref[...], preferred_element_type=jnp.float32)
    for k in range(3):

        @pl.when(step == k)
        def _(k=k):
            outs[2 * k][...] = terms[:half].astype(jnp.bfloat16)
            outs[2 * k + 1][...] = terms[half:].astype(jnp.bfloat16)

    @pl.when(step == 3)
    def _():
        outs[6][...] = terms + base_ref[...].astype(jnp.float32)


def project(places, rows, weight, base):
    tok, inner = rows.shape
    width = base.shape[1]
    piece = pl.BlockSpec((tok // 2, width), lambda j, o: (0, 0))
    whole = pl.BlockSpec((tok, width), lambda j, o: (0, 0))
    outs = pl.pallas_call(
        project_kernel,
        grid_spec=pltpu.PrefetchScalarGridSpec(
            num_scalar_prefetch=1,
            grid=(4,),
            in_specs=[
                pl.BlockSpec((tok, inner), lambda j, o: (0, 0)),
                pl.BlockSpec((inner, width), lambda j, o: (0, o[j])),
                whole,
            ],
            out_specs=[piece] * 6 + [whole],
        ),
        out_shape=[jax.ShapeDtypeStruct((tok // 2, width), jnp.bfloat16)] * 6
        + [jax.ShapeDtypeStruct((tok, width), jnp.float32)],
        cost_estimate=pl.CostEstimate(
            flops=8 * tok * inner * width,
            bytes_accessed=2 * tok * inner + 8 * inner * width + 12 * tok * width,
            transcendentals=0,
        ),
        compiler_params=pltpu.CompilerParams(vmem_limit_bytes=24 << 20),
        name="project",
    )(places, rows, weight, base)
    return (outs[0:2], outs[2:4], outs[4:6], outs[6])


def norm_kernel(places_ref, gain_ref, own_ref, left_ref, right_ref, top_ref, low_ref, out_ref):
    width = own_ref.shape[1]
    half = top_ref.shape[0]
    model = out_ref.shape[1]
    for at, far_ref in ((0, top_ref), (half, low_ref)):
        parts = [
            ref[pl.ds(at, half), :].astype(jnp.float32) for ref in (own_ref, left_ref, right_ref)
        ]
        parts = [far_ref[...].astype(jnp.float32), parts[2], parts[1], parts[0]]
        square = sum(jnp.sum(p * p, axis=-1, keepdims=True) for p in parts)
        scale = lax.rsqrt(square / model + 1e-06)
        for k, part in enumerate(parts):
            place = places_ref[k]
            gain = gain_ref[pl.ds(place, 1), :]
            columns = pl.ds(pl.multiple_of(place * width, width), width)
            out_ref[pl.ds(at, half), columns] = (part * scale * gain).astype(out_ref.dtype)


def normalised(places, gain, own, axis):
    tok, width = own.shape
    half = tok // 2
    left, right = (shifted(own, axis, 1), shifted(own, axis, -1))
    far_top = shifted(left[:half], axis, 1)
    far_low = shifted(right[half:], axis, -1)
    vmem = pl.BlockSpec(memory_space=pltpu.VMEM)
    model = gain.shape[0]
    return pl.pallas_call(
        norm_kernel,
        in_specs=[pl.BlockSpec(memory_space=pltpu.SMEM)] + [vmem] * 6,
        out_specs=vmem,
        out_shape=jax.ShapeDtypeStruct((tok, model), jnp.bfloat16),
        cost_estimate=pl.CostEstimate(
            flops=6 * tok * model, bytes_accessed=4 * tok * model, transcendentals=tok
        ),
        compiler_params=pltpu.CompilerParams(vmem_limit_bytes=24 << 20),
        name="norm",
    )(places, gain.reshape(model // width, width), own, left, right, far_top, far_low)


def times_transposed(rows, columns):
    return lax.dot_general(
        rows, columns, (((1,), (1,)), ((), ())), preferred_element_type=jnp.float32
    )


def held(array):
    return pltpu.with_memory_space_constraint(array, pltpu.VMEM)


def hold(shape, dtype=jnp.bfloat16):
    return pltpu.VMEM(shape, dtype)


CHUNK = 256


def hide(normed_ref, both_ref, hidden_ref, low, at, size):
    rows = hidden_ref.shape[0]
    product = jnp.dot(
        normed_ref[low : low + rows, :],
        both_ref[:, pl.ds(2 * at, 2 * size)],
        preferred_element_type=jnp.float32,
    )
    gate = product[:, :size]
    up = product[:, size:]
    hidden_ref[:, pl.ds(at, size)] = (gate / (1.0 + jnp.exp(-gate)) * up).astype(jnp.bfloat16)


def two_shares(hidden_ref, down_ref, which, outs):
    def body(i, carry):
        terms = times_transposed(hidden_ref[...], down_ref[jnp.where(i == 0, *which)])
        for j in range(2):

            @pl.when(i == j)
            def _(j=j):
                outs[j][...] = terms.astype(jnp.bfloat16)

        return carry

    lax.fori_loop(0, 2, body, 0)


def top_kernel(places_ref, normed_ref, weights_ref, *rest):
    hidden_ref, far_ref, left_ref, both_ref, down_ref, sems, down_sems = rest
    units = hidden_ref.shape[1]
    owned = far_ref.shape[1]
    count, first = divmod(units, CHUNK)

    def copies(slot, at, size):
        return [
            pltpu.make_async_copy(
                weights_ref.at[:, pl.ds(k * units + at, size)],
                both_ref.at[:, pl.ds(2 * at + k * size, size)],
                sems.at[slot, k],
            )
            for k in range(2)
        ]

    def down_copy(k):
        row = pl.multiple_of(places_ref[k] * owned, owned)
        return pltpu.make_async_copy(
            weights_ref.at[pl.ds(row, owned), pl.ds(2 * units, units)],
            down_ref.at[k],
            down_sems.at[k],
        )

    for copy in copies(0, 0, first):
        copy.start()
    for i in range(count):
        for copy in copies(1 + i, first + i * CHUNK, CHUNK):
            copy.start()
    for k in range(4):
        down_copy(k).start()
    for copy in copies(0, 0, first):
        copy.wait()
    hide(normed_ref, both_ref, hidden_ref, 0, 0, first)

    def body(i, carry):
        at = pl.multiple_of(first + i * CHUNK, 128)
        for copy in copies(1 + i, at, CHUNK):
            copy.wait()
        hide(normed_ref, both_ref, hidden_ref, 0, at, CHUNK)
        return carry

    lax.fori_loop(0, count, body, 0)
    for k in range(4):
        down_copy(k).wait()
    two_shares(hidden_ref, down_ref, (0, 2), (far_ref, left_ref))


def low_kernel(normed_ref, both_ref, down_ref, hidden_ref, far_ref, right_ref):
    count, first = divmod(hidden_ref.shape[1], CHUNK)
    rows = hidden_ref.shape[0]
    hide(normed_ref, both_ref, hidden_ref, rows, 0, first)

    def body(i, carry):
        at = pl.multiple_of(first + i * CHUNK, 128)
        hide(normed_ref, both_ref, hidden_ref, rows, at, CHUNK)
        return carry

    lax.fori_loop(0, count, body, 0)
    two_shares(hidden_ref, down_ref, (0, 1), (far_ref, right_ref))


def rest_kernel(top_ref, low_ref, down_ref, right_ref, left_ref):
    right_ref[...] = times_transposed(top_ref[...], down_ref[1]).astype(jnp.bfloat16)
    left_ref[...] = times_transposed(low_ref[...], down_ref[2]).astype(jnp.bfloat16)


def own_kernel(top_ref, low_ref, down_ref, base_ref, out_ref):
    half = top_ref.shape[0]
    for at, hidden_ref in ((0, top_ref), (half, low_ref)):
        terms = times_transposed(hidden_ref[...], down_ref[3])
        out_ref[at : at + half] = terms + base_ref[at : at + half].astype(jnp.float32)


def feed_forward(places, normed, weights, base, axis):
    tok, model = normed.shape
    owned = base.shape[1]
    units = weights.shape[1] // 3
    half = tok // 2
    vmem = pl.BlockSpec(memory_space=pltpu.VMEM)
    part, hid = ((half, owned), (half, units))
    cost = pl.CostEstimate(
        flops=2 * tok * model * units, bytes_accessed=6 * model * units, transcendentals=half * units
    )
    small = pl.CostEstimate(
        flops=2 * tok * units * owned, bytes_accessed=4 * tok * owned, transcendentals=0
    )
    grant = pltpu.CompilerParams(vmem_limit_bytes=20 << 20)
    normed = held(normed)
    top, far_top, left_top, both, down = pl.pallas_call(
        top_kernel,
        in_specs=[
            pl.BlockSpec(memory_space=pltpu.SMEM),
            vmem,
            pl.BlockSpec(memory_space=pltpu.HBM),
        ],
        out_specs=[vmem] * 5,
        out_shape=[
            hold(hid),
            hold(part),
            hold(part),
            hold((model, 2 * units)),
            hold((4, owned, units)),
        ],
        scratch_shapes=[
            pltpu.SemaphoreType.DMA((1 + units // CHUNK, 2)),
            pltpu.SemaphoreType.DMA((4,)),
        ],
        cost_estimate=cost,
        compiler_params=grant,
        name="top",
    )(places, normed, weights)
    down = held(down)
    far_top_in = shifted(far_top, axis, 1)
    left_top_in = shifted(left_top, axis, -1)
    low_half = pl.pallas_call(
        low_kernel,
        in_specs=[vmem] * 3,
        out_specs=[vmem] * 3,
        out_shape=[hold(hid), hold(part), hold(part)],
        cost_estimate=cost,
        compiler_params=grant,
        name="low",
    )
    both = held(both)
    low, far_low, right_low = low_half(normed, both, down)
    far_low_in = shifted(far_low, axis, -1)
    right_low_in = shifted(right_low, axis, 1)
    top, low = (held(top), held(low))
    rest = pl.pallas_call(
        rest_kernel,
        in_specs=[vmem] * 3,
        out_specs=[vmem] * 2,
        out_shape=[hold(part)] * 2,
        cost_estimate=small,
        compiler_params=grant,
        name="rest",
    )
    right_top, left_low = rest(top, low, down)
    relay_top = relayed(far_top_in, right_top)
    relay_top_in = shifted(relay_top, axis, 1)
    relay_low = relayed(far_low_in, left_low)
    relay_low_in = shifted(relay_low, axis, -1)
    own = pl.pallas_call(
        own_kernel,
        in_specs=[vmem] * 4,
        out_specs=vmem,
        out_shape=hold((tok, owned), jnp.float32),
        cost_estimate=small,
        compiler_params=grant,
        name="own",
    )(top, low, down, base)
    return pl.pallas_call(
        settle_kernel,
        in_specs=[vmem] * 5,
        out_specs=vmem,
        out_shape=jax.ShapeDtypeStruct((tok, owned), jnp.bfloat16),
        cost_estimate=pl.CostEstimate(
            flops=2 * tok * owned, bytes_accessed=10 * tok * owned, transcendentals=0
        ),
        compiler_params=pltpu.CompilerParams(vmem_limit_bytes=12 << 20),
        name="close",
    )(held(own), left_top_in, relay_top_in, right_low_in, relay_low_in)


def rotate(values, positions):
    quarter = 16
    inverse = 10000.0 ** (-jnp.arange(quarter, dtype=jnp.float32) / quarter)

    def turn(part, place):
        angle = place.astype(jnp.float32)[:, None] * inverse[None, :]
        cosine = jnp.cos(angle)[:, None, :]
        sine = jnp.sin(angle)[:, None, :]
        first, second = (part[..., :quarter], part[..., quarter:])
        return jnp.concatenate(
            [first * cosine - second * sine, second * cosine + first * sine], axis=-1
        )

    grid_row = positions // GRID_W
    grid_col = positions % GRID_W
    return jnp.concatenate(
        [turn(values[..., :32], grid_row), turn(values[..., 32:], grid_col)], axis=-1
    )


def body(
    resid, queries, keys_values, sink, out_weight, norm_gain, gate_weight, up_weight, down_weight
):
    shard = jnp.concatenate((gate_weight, up_weight, down_weight.T), axis=1)
    weights = lax.all_gather(shard, "sp", axis=0, tiled=True)
    tok = queries.shape[0]
    heads_here = queries.shape[1] // HEAD_DIM
    kv_here = keys_values.shape[1]
    group = heads_here // kv_here
    offset = lax.axis_index("sp") * tok
    total_tokens = tok * lax.axis_size("sp")
    positions = offset + jnp.arange(tok, dtype=jnp.int32)
    rotated_q = rotate(
        queries.astype(jnp.float32).reshape(tok, heads_here, HEAD_DIM), positions
    ).astype(jnp.bfloat16)
    rotated_k = rotate(keys_values[..., :HEAD_DIM].astype(jnp.float32), positions).astype(
        jnp.bfloat16
    )
    joined = jnp.concatenate([rotated_k, keys_values[..., HEAD_DIM:]], axis=-1)
    padded = with_halo(joined, (("sp", 0),), WINDOW)
    blocks = tok // WINDOW
    key_blocks = jnp.stack(
        [padded[index * WINDOW : index * WINDOW + 3 * WINDOW] for index in range(blocks)]
    )
    grouped = rotated_q.reshape(blocks, WINDOW, kv_here, group, HEAD_DIM)
    scores = jnp.einsum(
        "nqkgd,njkd->nkgqj", grouped, key_blocks[..., :HEAD_DIM], preferred_element_type=jnp.float32
    ) * HEAD_DIM ** (-0.5)
    block_start = offset + WINDOW * jnp.arange(blocks, dtype=jnp.int32)
    query_pos = block_start[:, None] + jnp.arange(WINDOW, dtype=jnp.int32)[None, :]
    key_pos = block_start[:, None] - WINDOW + jnp.arange(3 * WINDOW, dtype=jnp.int32)[None, :]
    valid = (
        (jnp.abs(query_pos[:, :, None] - key_pos[:, None, :]) <= WINDOW)
        & (key_pos[:, None, :] >= 0)
        & (key_pos[:, None, :] < total_tokens)
    )
    scores = jnp.where(valid[:, None, None], scores, jnp.float32(-1e30))
    sink_grid = sink.reshape(kv_here, group)[None, :, :, None]
    top = jnp.maximum(jnp.max(scores, axis=-1), sink_grid)
    expo = jnp.exp(scores - top[..., None])
    denom = jnp.sum(expo, axis=-1) + jnp.exp(sink_grid - top)
    probs = (expo / denom[..., None]).astype(jnp.bfloat16)
    attended = jnp.einsum(
        "nkgqj,njkd->nqkgd", probs, key_blocks[..., HEAD_DIM:], preferred_element_type=jnp.float32
    )
    attended = attended.astype(jnp.bfloat16).reshape(tok, heads_here * HEAD_DIM)
    places = ring_places("tp")
    far, right, left, own = project(places, attended, out_weight, resid)
    stream = ring_sum(far, right, left, own, "tp")
    normed = normalised(places, norm_gain, stream, "tp")
    return feed_forward(places, normed, weights, stream, "tp")


def solution(mesh):
    return jax.shard_map(
        body,
        mesh=mesh,
        in_specs=(
            P(("grp", "sp"), "tp"),
            P(("grp", "sp"), "tp"),
            P(("grp", "sp"), "tp", None),
            P("tp"),
            P("tp", None),
            P(),
            P("sp", "tp"),
            P("sp", "tp"),
            P("tp", "sp"),
        ),
        out_specs=P(("grp", "sp"), "tp"),
        check_vma=False,
    )
```

```python
import jax
import jax.numpy as jnp
from jax import lax
from jax.experimental import pallas as pl
from jax.experimental.pallas import tpu as pltpu
from jax.sharding import PartitionSpec as P


HEAD_DIM = 64
WINDOW = 128
GRID_W = 64


def with_halo(cells, sides, width):
    for axis, dim in sides:
        count = lax.axis_size(axis)
        ends = count - 1
        head = lax.slice_in_dim(cells, 0, width, axis=dim)
        tail = lax.slice_in_dim(cells, cells.shape[dim] - width, cells.shape[dim], axis=dim)
        cells = jnp.concatenate(
            [
                lax.ppermute(tail, axis, [(i, (i + 1) % count) for i in range(ends)]),
                cells,
                lax.ppermute(head, axis, [((i + 1) % count, i) for i in range(ends)]),
            ],
            axis=dim,
        )
    return cells


def shifted(array, axis, by):
    count = lax.axis_size(axis)
    return lax.ppermute(array, axis, [(i, (i + by) % count) for i in range(count)])


def added(*terms):
    return sum((t.astype(jnp.float32) for t in terms[1:]), terms[0].astype(jnp.float32))


def settle_kernel(own_ref, top_ref, top2_ref, low_ref, low2_ref, out_ref):
    half = top_ref.shape[0]
    out_ref[:half] = added(own_ref[:half], top_ref[...], top2_ref[...]).astype(out_ref.dtype)
    out_ref[half:] = added(own_ref[half:], low_ref[...], low2_ref[...]).astype(out_ref.dtype)


def settle(own, tops, lows):
    vmem = pl.BlockSpec(memory_space=pltpu.VMEM)
    return pl.pallas_call(
        settle_kernel,
        in_specs=[vmem] * 5,
        out_specs=vmem,
        out_shape=jax.ShapeDtypeStruct(own.shape, jnp.bfloat16),
        cost_estimate=pl.CostEstimate(
            flops=2 * own.size, bytes_accessed=10 * own.size, transcendentals=0
        ),
        compiler_params=pltpu.CompilerParams(vmem_limit_bytes=12 << 20),
        name="settle",
    )(own, *tops, *lows)


def relayed(far_in, mine):
    return added(mine, far_in).astype(jnp.bfloat16)


def ring_places(axis):
    count = lax.axis_size(axis)
    me = lax.axis_index(axis)
    return jnp.stack([(me + by) % count for by in (2, 1, count - 1, 0)]).astype(jnp.int32)


def ring_sum(far, right, left, own, axis):
    far_top_in = shifted(far[0], axis, 1)
    far_low_in = shifted(far[1], axis, -1)
    right_low_in = shifted(right[1], axis, 1)
    left_top_in = shifted(left[0], axis, -1)
    relay_top_in = shifted(relayed(far_top_in, right[0]), axis, 1)
    relay_low_in = shifted(relayed(far_low_in, left[1]), axis, -1)
    return settle(own, (left_top_in, relay_top_in), (right_low_in, relay_low_in))


def project_kernel(places_ref, rows_ref, weight_ref, base_ref, *outs):
    half = outs[0].shape[0]
    step = pl.program_id(0)
    terms = jnp.dot(rows_ref[...], weight_ref[...], preferred_element_type=jnp.float32)
    for k in range(3):

        @pl.when(step == k)
        def _(k=k):
            outs[2 * k][...] = terms[:half].astype(jnp.bfloat16)
            outs[2 * k + 1][...] = terms[half:].astype(jnp.bfloat16)

    @pl.when(step == 3)
    def _():
        outs[6][...] = terms + base_ref[...].astype(jnp.float32)


def project(places, rows, weight, base):
    tok, inner = rows.shape
    width = base.shape[1]
    piece = pl.BlockSpec((tok // 2, width), lambda j, o: (0, 0))
    whole = pl.BlockSpec((tok, width), lambda j, o: (0, 0))
    outs = pl.pallas_call(
        project_kernel,
        grid_spec=pltpu.PrefetchScalarGridSpec(
            num_scalar_prefetch=1,
            grid=(4,),
            in_specs=[
                pl.BlockSpec((tok, inner), lambda j, o: (0, 0)),
                pl.BlockSpec((inner, width), lambda j, o: (0, o[j])),
                whole,
            ],
            out_specs=[piece] * 6 + [whole],
        ),
        out_shape=[jax.ShapeDtypeStruct((tok // 2, width), jnp.bfloat16)] * 6
        + [jax.ShapeDtypeStruct((tok, width), jnp.float32)],
        cost_estimate=pl.CostEstimate(
            flops=8 * tok * inner * width,
            bytes_accessed=2 * tok * inner + 8 * inner * width + 12 * tok * width,
            transcendentals=0,
        ),
        compiler_params=pltpu.CompilerParams(vmem_limit_bytes=24 << 20),
        name="project",
    )(places, rows, weight, base)
    return (outs[0:2], outs[2:4], outs[4:6], outs[6])


def norm_kernel(places_ref, gain_ref, own_ref, left_ref, right_ref, top_ref, low_ref, out_ref):
    width = own_ref.shape[1]
    half = top_ref.shape[0]
    model = out_ref.shape[1]
    for at, far_ref in ((0, top_ref), (half, low_ref)):
        parts = [
            ref[pl.ds(at, half), :].astype(jnp.float32) for ref in (own_ref, left_ref, right_ref)
        ]
        parts = [far_ref[...].astype(jnp.float32), parts[2], parts[1], parts[0]]
        square = sum(jnp.sum(p * p, axis=-1, keepdims=True) for p in parts)
        scale = lax.rsqrt(square / model + 1e-06)
        for k, part in enumerate(parts):
            place = places_ref[k]
            gain = gain_ref[pl.ds(place, 1), :]
            columns = pl.ds(pl.multiple_of(place * width, width), width)
            out_ref[pl.ds(at, half), columns] = (part * scale * gain).astype(out_ref.dtype)


def normalised(places, gain, own, axis):
    tok, width = own.shape
    half = tok // 2
    left, right = (shifted(own, axis, 1), shifted(own, axis, -1))
    far_top = shifted(left[:half], axis, 1)
    far_low = shifted(right[half:], axis, -1)
    vmem = pl.BlockSpec(memory_space=pltpu.VMEM)
    model = gain.shape[0]
    return pl.pallas_call(
        norm_kernel,
        in_specs=[pl.BlockSpec(memory_space=pltpu.SMEM)] + [vmem] * 6,
        out_specs=vmem,
        out_shape=jax.ShapeDtypeStruct((tok, model), jnp.bfloat16),
        cost_estimate=pl.CostEstimate(
            flops=6 * tok * model, bytes_accessed=4 * tok * model, transcendentals=tok
        ),
        compiler_params=pltpu.CompilerParams(vmem_limit_bytes=24 << 20),
        name="norm",
    )(places, gain.reshape(model // width, width), own, left, right, far_top, far_low)


def times_transposed(rows, columns):
    return lax.dot_general(
        rows, columns, (((1,), (1,)), ((), ())), preferred_element_type=jnp.float32
    )


def held(array):
    return pltpu.with_memory_space_constraint(array, pltpu.VMEM)


def hold(shape, dtype=jnp.bfloat16):
    return pltpu.VMEM(shape, dtype)


CHUNK = 256


def hide(normed_ref, both_ref, hidden_ref, low, at, size):
    rows = hidden_ref.shape[0]
    product = jnp.dot(
        normed_ref[low : low + rows, :],
        both_ref[:, pl.ds(2 * at, 2 * size)],
        preferred_element_type=jnp.float32,
    )
    gate = product[:, :size]
    up = product[:, size:]
    hidden_ref[:, pl.ds(at, size)] = (gate / (1.0 + jnp.exp(-gate)) * up).astype(jnp.bfloat16)


def two_shares(hidden_ref, down_ref, which, outs):
    def body(i, carry):
        terms = times_transposed(hidden_ref[...], down_ref[jnp.where(i == 0, *which)])
        for j in range(2):

            @pl.when(i == j)
            def _(j=j):
                outs[j][...] = terms.astype(jnp.bfloat16)

        return carry

    lax.fori_loop(0, 2, body, 0)


def top_kernel(places_ref, normed_ref, weights_ref, *rest):
    hidden_ref, far_ref, left_ref, both_ref, down_ref, sems, down_sems = rest
    units = hidden_ref.shape[1]
    owned = far_ref.shape[1]
    count, first = divmod(units, CHUNK)

    def copies(slot, at, size):
        return [
            pltpu.make_async_copy(
                weights_ref.at[:, pl.ds(k * units + at, size)],
                both_ref.at[:, pl.ds(2 * at + k * size, size)],
                sems.at[slot, k],
            )
            for k in range(2)
        ]

    def down_copy(k):
        row = pl.multiple_of(places_ref[k] * owned, owned)
        return pltpu.make_async_copy(
            weights_ref.at[pl.ds(row, owned), pl.ds(2 * units, units)],
            down_ref.at[k],
            down_sems.at[k],
        )

    for copy in copies(0, 0, first):
        copy.start()
    for i in range(count):
        for copy in copies(1 + i, first + i * CHUNK, CHUNK):
            copy.start()
    for k in range(4):
        down_copy(k).start()
    for copy in copies(0, 0, first):
        copy.wait()
    hide(normed_ref, both_ref, hidden_ref, 0, 0, first)

    def body(i, carry):
        at = pl.multiple_of(first + i * CHUNK, 128)
        for copy in copies(1 + i, at, CHUNK):
            copy.wait()
        hide(normed_ref, both_ref, hidden_ref, 0, at, CHUNK)
        return carry

    lax.fori_loop(0, count, body, 0)
    for k in range(4):
        down_copy(k).wait()
    two_shares(hidden_ref, down_ref, (0, 2), (far_ref, left_ref))


def low_kernel(normed_ref, both_ref, down_ref, hidden_ref, far_ref, right_ref):
    count, first = divmod(hidden_ref.shape[1], CHUNK)
    rows = hidden_ref.shape[0]
    low = normed_ref.shape[0] - rows
    hide(normed_ref, both_ref, hidden_ref, low, 0, first)

    def body(i, carry):
        at = pl.multiple_of(first + i * CHUNK, 128)
        hide(normed_ref, both_ref, hidden_ref, low, at, CHUNK)
        return carry

    lax.fori_loop(0, count, body, 0)
    two_shares(hidden_ref, down_ref, (0, 1), (far_ref, right_ref))


def rest_kernel(top_ref, low_ref, down_ref, right_ref, left_ref):
    right_ref[...] = times_transposed(top_ref[...], down_ref[1]).astype(jnp.bfloat16)
    left_ref[...] = times_transposed(low_ref[...], down_ref[2]).astype(jnp.bfloat16)


def own_kernel(top_ref, low_ref, down_ref, base_ref, out_ref):
    half = top_ref.shape[0]
    for rows, hidden_ref in ((slice(None, half), top_ref), (slice(half, None), low_ref)):
        terms = times_transposed(hidden_ref[...], down_ref[3])
        out_ref[rows] = terms + base_ref[rows].astype(jnp.float32)


def feed_forward(places, normed, weights, base, axis):
    tok, model = normed.shape
    owned = base.shape[1]
    units = weights.shape[1] // 3
    vmem = pl.BlockSpec(memory_space=pltpu.VMEM)
    first = tok * 11 // 20
    part, hid = ((first, owned), (first, units))
    low_part, low_hid = ((tok - first, owned), (tok - first, units))
    cost = pl.CostEstimate(
        flops=2 * tok * model * units, bytes_accessed=6 * model * units, transcendentals=tok // 2 * units
    )
    small = pl.CostEstimate(
        flops=2 * tok * units * owned, bytes_accessed=4 * tok * owned, transcendentals=0
    )
    grant = pltpu.CompilerParams(vmem_limit_bytes=20 << 20)
    normed = held(normed)
    top, far_top, left_top, both, down = pl.pallas_call(
        top_kernel,
        in_specs=[
            pl.BlockSpec(memory_space=pltpu.SMEM),
            vmem,
            pl.BlockSpec(memory_space=pltpu.HBM),
        ],
        out_specs=[vmem] * 5,
        out_shape=[
            hold(hid),
            hold(part),
            hold(part),
            hold((model, 2 * units)),
            hold((4, owned, units)),
        ],
        scratch_shapes=[
            pltpu.SemaphoreType.DMA((1 + units // CHUNK, 2)),
            pltpu.SemaphoreType.DMA((4,)),
        ],
        cost_estimate=cost,
        compiler_params=grant,
        name="top",
    )(places, normed, weights)
    down = held(down)
    far_top_in = shifted(far_top, axis, 1)
    left_top_in = shifted(left_top, axis, -1)
    low_half = pl.pallas_call(
        low_kernel,
        in_specs=[vmem] * 3,
        out_specs=[vmem] * 3,
        out_shape=[hold(low_hid), hold(low_part), hold(low_part)],
        cost_estimate=cost,
        compiler_params=grant,
        name="low",
    )
    both = held(both)
    low, far_low, right_low = low_half(normed, both, down)
    far_low_in = shifted(far_low, axis, -1)
    right_low_in = shifted(right_low, axis, 1)
    top, low = (held(top), held(low))
    rest = pl.pallas_call(
        rest_kernel,
        in_specs=[vmem] * 3,
        out_specs=[vmem] * 2,
        out_shape=[hold(part), hold(low_part)],
        cost_estimate=small,
        compiler_params=grant,
        name="rest",
    )
    right_top, left_low = rest(top, low, down)
    relay_top = relayed(far_top_in, right_top)
    relay_top_in = shifted(relay_top, axis, 1)
    relay_low = relayed(far_low_in, left_low)
    relay_low_in = shifted(relay_low, axis, -1)
    own = pl.pallas_call(
        own_kernel,
        in_specs=[vmem] * 4,
        out_specs=vmem,
        out_shape=hold((tok, owned), jnp.float32),
        cost_estimate=small,
        compiler_params=grant,
        name="own",
    )(top, low, down, base)
    return pl.pallas_call(
        settle_kernel,
        in_specs=[vmem] * 5,
        out_specs=vmem,
        out_shape=jax.ShapeDtypeStruct((tok, owned), jnp.bfloat16),
        cost_estimate=pl.CostEstimate(
            flops=2 * tok * owned, bytes_accessed=10 * tok * owned, transcendentals=0
        ),
        compiler_params=pltpu.CompilerParams(vmem_limit_bytes=12 << 20),
        name="close",
    )(held(own), left_top_in, relay_top_in, right_low_in, relay_low_in)


def rotate(values, positions):
    quarter = 16
    inverse = 10000.0 ** (-jnp.arange(quarter, dtype=jnp.float32) / quarter)

    def turn(part, place):
        angle = place.astype(jnp.float32)[:, None] * inverse[None, :]
        cosine = jnp.cos(angle)[:, None, :]
        sine = jnp.sin(angle)[:, None, :]
        first, second = (part[..., :quarter], part[..., quarter:])
        return jnp.concatenate(
            [first * cosine - second * sine, second * cosine + first * sine], axis=-1
        )

    grid_row = positions // GRID_W
    grid_col = positions % GRID_W
    return jnp.concatenate(
        [turn(values[..., :32], grid_row), turn(values[..., 32:], grid_col)], axis=-1
    )


def body(
    resid, queries, keys_values, sink, out_weight, norm_gain, gate_weight, up_weight, down_weight
):
    shard = jnp.concatenate((gate_weight, up_weight, down_weight.T), axis=1)
    weights = lax.all_gather(shard, "sp", axis=0, tiled=True)
    tok = queries.shape[0]
    heads_here = queries.shape[1] // HEAD_DIM
    kv_here = keys_values.shape[1]
    group = heads_here // kv_here
    offset = lax.axis_index("sp") * tok
    total_tokens = tok * lax.axis_size("sp")
    positions = offset + jnp.arange(tok, dtype=jnp.int32)
    rotated_q = rotate(
        queries.astype(jnp.float32).reshape(tok, heads_here, HEAD_DIM), positions
    ).astype(jnp.bfloat16)
    rotated_k = rotate(keys_values[..., :HEAD_DIM].astype(jnp.float32), positions).astype(
        jnp.bfloat16
    )
    joined = jnp.concatenate([rotated_k, keys_values[..., HEAD_DIM:]], axis=-1)
    padded = with_halo(joined, (("sp", 0),), WINDOW)
    blocks = tok // WINDOW
    key_blocks = jnp.stack(
        [padded[index * WINDOW : index * WINDOW + 3 * WINDOW] for index in range(blocks)]
    )
    grouped = rotated_q.reshape(blocks, WINDOW, kv_here, group, HEAD_DIM)
    scores = jnp.einsum(
        "nqkgd,njkd->nkgqj", grouped, key_blocks[..., :HEAD_DIM], preferred_element_type=jnp.float32
    ) * HEAD_DIM ** (-0.5)
    block_start = offset + WINDOW * jnp.arange(blocks, dtype=jnp.int32)
    query_pos = block_start[:, None] + jnp.arange(WINDOW, dtype=jnp.int32)[None, :]
    key_pos = block_start[:, None] - WINDOW + jnp.arange(3 * WINDOW, dtype=jnp.int32)[None, :]
    valid = (
        (jnp.abs(query_pos[:, :, None] - key_pos[:, None, :]) <= WINDOW)
        & (key_pos[:, None, :] >= 0)
        & (key_pos[:, None, :] < total_tokens)
    )
    scores = jnp.where(valid[:, None, None], scores, jnp.float32(-1e30))
    sink_grid = sink.reshape(kv_here, group)[None, :, :, None]
    top = jnp.maximum(jnp.max(scores, axis=-1), sink_grid)
    expo = jnp.exp(scores - top[..., None])
    denom = jnp.sum(expo, axis=-1) + jnp.exp(sink_grid - top)
    probs = (expo / denom[..., None]).astype(jnp.bfloat16)
    attended = jnp.einsum(
        "nkgqj,njkd->nqkgd", probs, key_blocks[..., HEAD_DIM:], preferred_element_type=jnp.float32
    )
    attended = attended.astype(jnp.bfloat16).reshape(tok, heads_here * HEAD_DIM)
    places = ring_places("tp")
    far, right, left, own = project(places, attended, out_weight, resid)
    stream = ring_sum(far, right, left, own, "tp")
    normed = normalised(places, norm_gain, stream, "tp")
    return feed_forward(places, normed, weights, stream, "tp")


def solution(mesh):
    return jax.shard_map(
        body,
        mesh=mesh,
        in_specs=(
            P(("grp", "sp"), "tp"),
            P(("grp", "sp"), "tp"),
            P(("grp", "sp"), "tp", None),
            P("tp"),
            P("tp", None),
            P(),
            P("sp", "tp"),
            P("sp", "tp"),
            P("tp", "sp"),
        ),
        out_specs=P(("grp", "sp"), "tp"),
        check_vma=False,
    )
```

```python
import jax
import jax.numpy as jnp
from jax import lax
from jax.experimental import pallas as pl
from jax.experimental.pallas import tpu as pltpu
from jax.sharding import PartitionSpec as P


HEAD_DIM = 64
WINDOW = 128
GRID_W = 64


def with_halo(cells, sides, width):
    for axis, dim in sides:
        count = lax.axis_size(axis)
        ends = count - 1
        head = lax.slice_in_dim(cells, 0, width, axis=dim)
        tail = lax.slice_in_dim(cells, cells.shape[dim] - width, cells.shape[dim], axis=dim)
        cells = jnp.concatenate(
            [
                lax.ppermute(tail, axis, [(i, (i + 1) % count) for i in range(ends)]),
                cells,
                lax.ppermute(head, axis, [((i + 1) % count, i) for i in range(ends)]),
            ],
            axis=dim,
        )
    return cells


def shifted(array, axis, by):
    count = lax.axis_size(axis)
    return lax.ppermute(array, axis, [(i, (i + by) % count) for i in range(count)])


def added(*terms):
    return sum((t.astype(jnp.float32) for t in terms[1:]), terms[0].astype(jnp.float32))


def settle_kernel(own_ref, top_ref, top2_ref, low_ref, low2_ref, out_ref):
    half = top_ref.shape[0]
    out_ref[:half] = added(own_ref[:half], top_ref[...], top2_ref[...]).astype(out_ref.dtype)
    out_ref[half:] = added(own_ref[half:], low_ref[...], low2_ref[...]).astype(out_ref.dtype)


def settle(own, tops, lows):
    vmem = pl.BlockSpec(memory_space=pltpu.VMEM)
    return pl.pallas_call(
        settle_kernel,
        in_specs=[vmem] * 5,
        out_specs=vmem,
        out_shape=jax.ShapeDtypeStruct(own.shape, jnp.bfloat16),
        cost_estimate=pl.CostEstimate(
            flops=2 * own.size, bytes_accessed=10 * own.size, transcendentals=0
        ),
        compiler_params=pltpu.CompilerParams(vmem_limit_bytes=12 << 20),
        name="settle",
    )(own, *tops, *lows)


def relayed(far_in, mine):
    return added(mine, far_in).astype(jnp.bfloat16)


def ring_places(axis):
    count = lax.axis_size(axis)
    me = lax.axis_index(axis)
    return jnp.stack([(me + by) % count for by in (2, 1, count - 1, 0)]).astype(jnp.int32)


def ring_sum(far, right, left, own, axis):
    far_top_in = shifted(far[0], axis, 1)
    far_low_in = shifted(far[1], axis, -1)
    right_low_in = shifted(right[1], axis, 1)
    left_top_in = shifted(left[0], axis, -1)
    relay_top_in = shifted(relayed(far_top_in, right[0]), axis, 1)
    relay_low_in = shifted(relayed(far_low_in, left[1]), axis, -1)
    return settle(own, (left_top_in, relay_top_in), (right_low_in, relay_low_in))


def project_kernel(places_ref, rows_ref, weight_ref, base_ref, *outs):
    half = outs[0].shape[0]
    step = pl.program_id(0)
    terms = jnp.dot(rows_ref[...], weight_ref[...], preferred_element_type=jnp.float32)
    for k in range(3):

        @pl.when(step == k)
        def _(k=k):
            outs[2 * k][...] = terms[:half].astype(jnp.bfloat16)
            outs[2 * k + 1][...] = terms[half:].astype(jnp.bfloat16)

    @pl.when(step == 3)
    def _():
        outs[6][...] = terms + base_ref[...].astype(jnp.float32)


def project(places, rows, weight, base):
    tok, inner = rows.shape
    width = base.shape[1]
    piece = pl.BlockSpec((tok // 2, width), lambda j, o: (0, 0))
    whole = pl.BlockSpec((tok, width), lambda j, o: (0, 0))
    outs = pl.pallas_call(
        project_kernel,
        grid_spec=pltpu.PrefetchScalarGridSpec(
            num_scalar_prefetch=1,
            grid=(4,),
            in_specs=[
                pl.BlockSpec((tok, inner), lambda j, o: (0, 0)),
                pl.BlockSpec((inner, width), lambda j, o: (0, o[j])),
                whole,
            ],
            out_specs=[piece] * 6 + [whole],
        ),
        out_shape=[jax.ShapeDtypeStruct((tok // 2, width), jnp.bfloat16)] * 6
        + [jax.ShapeDtypeStruct((tok, width), jnp.float32)],
        cost_estimate=pl.CostEstimate(
            flops=8 * tok * inner * width,
            bytes_accessed=2 * tok * inner + 8 * inner * width + 12 * tok * width,
            transcendentals=0,
        ),
        compiler_params=pltpu.CompilerParams(vmem_limit_bytes=24 << 20),
        name="project",
    )(places, rows, weight, base)
    return (outs[0:2], outs[2:4], outs[4:6], outs[6])


def norm_kernel(places_ref, gain_ref, own_ref, left_ref, right_ref, top_ref, low_ref, out_ref):
    width = own_ref.shape[1]
    half = top_ref.shape[0]
    model = out_ref.shape[1]
    for at, far_ref in ((0, top_ref), (half, low_ref)):
        parts = [
            ref[pl.ds(at, half), :].astype(jnp.float32) for ref in (own_ref, left_ref, right_ref)
        ]
        parts = [far_ref[...].astype(jnp.float32), parts[2], parts[1], parts[0]]
        square = sum(jnp.sum(p * p, axis=-1, keepdims=True) for p in parts)
        scale = lax.rsqrt(square / model + 1e-06)
        for k, part in enumerate(parts):
            place = places_ref[k]
            gain = gain_ref[pl.ds(place, 1), :]
            columns = pl.ds(pl.multiple_of(place * width, width), width)
            out_ref[pl.ds(at, half), columns] = (part * scale * gain).astype(out_ref.dtype)


def normalised(places, gain, own, axis):
    tok, width = own.shape
    half = tok // 2
    left, right = (shifted(own, axis, 1), shifted(own, axis, -1))
    far_top = shifted(left[:half], axis, 1)
    far_low = shifted(right[half:], axis, -1)
    vmem = pl.BlockSpec(memory_space=pltpu.VMEM)
    model = gain.shape[0]
    return pl.pallas_call(
        norm_kernel,
        in_specs=[pl.BlockSpec(memory_space=pltpu.SMEM)] + [vmem] * 6,
        out_specs=vmem,
        out_shape=jax.ShapeDtypeStruct((tok, model), jnp.bfloat16),
        cost_estimate=pl.CostEstimate(
            flops=6 * tok * model, bytes_accessed=4 * tok * model, transcendentals=tok
        ),
        compiler_params=pltpu.CompilerParams(vmem_limit_bytes=24 << 20),
        name="norm",
    )(places, gain.reshape(model // width, width), own, left, right, far_top, far_low)


def times_transposed(rows, columns):
    return lax.dot_general(
        rows, columns, (((1,), (1,)), ((), ())), preferred_element_type=jnp.float32
    )


def held(array):
    return pltpu.with_memory_space_constraint(array, pltpu.VMEM)


def hold(shape, dtype=jnp.bfloat16):
    return pltpu.VMEM(shape, dtype)


CHUNK = 256
BLOCKS = 4


def hide(normed_ref, both_ref, hidden_ref, low, at, size):
    rows = hidden_ref.shape[0]
    product = jnp.dot(
        normed_ref[low : low + rows, :],
        both_ref[:, pl.ds(2 * at, 2 * size)],
        preferred_element_type=jnp.float32,
    )
    gate = product[:, :size]
    up = product[:, size:]
    hidden_ref[:, pl.ds(at, size)] = (gate / (1.0 + jnp.exp(-gate)) * up).astype(jnp.bfloat16)


def two_shares(hidden_ref, down_ref, which, outs):
    def body(i, carry):
        terms = times_transposed(hidden_ref[...], down_ref[jnp.where(i == 0, *which)])
        for j in range(2):

            @pl.when(i == j)
            def _(j=j):
                outs[j][...] = terms.astype(jnp.bfloat16)

        return carry

    lax.fori_loop(0, 2, body, 0)


def top_kernel(places_ref, normed_ref, weights_ref, *rest):
    hidden_ref, far_ref, left_ref, both_ref, down_ref, sems, down_sems = rest
    units = hidden_ref.shape[1]
    owned = far_ref.shape[1]
    deep = both_ref.shape[0] // BLOCKS
    count, first = divmod(units, CHUNK)

    def copies(slot, at, size):
        return [
            pltpu.make_async_copy(
                weights_ref.at[pl.ds(block * deep, deep), pl.ds(k * units + at, size)],
                both_ref.at[pl.ds(block * deep, deep), pl.ds(2 * at + k * size, size)],
                sems.at[slot, k, block],
            )
            for k in range(2)
            for block in range(BLOCKS)
        ]

    def down_copy(k):
        row = pl.multiple_of(places_ref[k] * owned, owned)
        return pltpu.make_async_copy(
            weights_ref.at[pl.ds(row, owned), pl.ds(2 * units, units)],
            down_ref.at[k],
            down_sems.at[k],
        )

    for copy in copies(0, 0, first):
        copy.start()
    for i in range(count):
        for copy in copies(1 + i, first + i * CHUNK, CHUNK):
            copy.start()
    for k in range(4):
        down_copy(k).start()
    for copy in copies(0, 0, first):
        copy.wait()
    hide(normed_ref, both_ref, hidden_ref, 0, 0, first)

    def body(i, carry):
        at = pl.multiple_of(first + i * CHUNK, 128)
        for copy in copies(1 + i, at, CHUNK):
            copy.wait()
        hide(normed_ref, both_ref, hidden_ref, 0, at, CHUNK)
        return carry

    lax.fori_loop(0, count, body, 0)
    for k in range(4):
        down_copy(k).wait()
    two_shares(hidden_ref, down_ref, (0, 2), (far_ref, left_ref))


def low_kernel(normed_ref, both_ref, down_ref, hidden_ref, far_ref, right_ref):
    count, first = divmod(hidden_ref.shape[1], CHUNK)
    rows = hidden_ref.shape[0]
    low = normed_ref.shape[0] - rows
    hide(normed_ref, both_ref, hidden_ref, low, 0, first)

    def body(i, carry):
        at = pl.multiple_of(first + i * CHUNK, 128)
        hide(normed_ref, both_ref, hidden_ref, low, at, CHUNK)
        return carry

    lax.fori_loop(0, count, body, 0)
    two_shares(hidden_ref, down_ref, (0, 1), (far_ref, right_ref))


def rest_kernel(top_ref, low_ref, down_ref, right_ref, left_ref):
    right_ref[...] = times_transposed(top_ref[...], down_ref[1]).astype(jnp.bfloat16)
    left_ref[...] = times_transposed(low_ref[...], down_ref[2]).astype(jnp.bfloat16)


def own_kernel(top_ref, low_ref, down_ref, base_ref, out_ref):
    half = top_ref.shape[0]
    for rows, hidden_ref in ((slice(None, half), top_ref), (slice(half, None), low_ref)):
        terms = times_transposed(hidden_ref[...], down_ref[3])
        out_ref[rows] = terms + base_ref[rows].astype(jnp.float32)


def feed_forward(places, normed, weights, base, axis):
    tok, model = normed.shape
    owned = base.shape[1]
    units = weights.shape[1] // 3
    vmem = pl.BlockSpec(memory_space=pltpu.VMEM)
    first = tok * 11 // 20
    part, hid = ((first, owned), (first, units))
    low_part, low_hid = ((tok - first, owned), (tok - first, units))
    cost = pl.CostEstimate(
        flops=2 * tok * model * units, bytes_accessed=6 * model * units, transcendentals=tok // 2 * units
    )
    small = pl.CostEstimate(
        flops=2 * tok * units * owned, bytes_accessed=4 * tok * owned, transcendentals=0
    )
    grant = pltpu.CompilerParams(vmem_limit_bytes=20 << 20)
    normed = held(normed)
    top, far_top, left_top, both, down = pl.pallas_call(
        top_kernel,
        in_specs=[
            pl.BlockSpec(memory_space=pltpu.SMEM),
            vmem,
            pl.BlockSpec(memory_space=pltpu.HBM),
        ],
        out_specs=[vmem] * 5,
        out_shape=[
            hold(hid),
            hold(part),
            hold(part),
            hold((model, 2 * units)),
            hold((4, owned, units)),
        ],
        scratch_shapes=[
            pltpu.SemaphoreType.DMA((1 + units // CHUNK, 2, BLOCKS)),
            pltpu.SemaphoreType.DMA((4,)),
        ],
        cost_estimate=cost,
        compiler_params=grant,
        name="top",
    )(places, normed, weights)
    down = held(down)
    far_top_in = shifted(far_top, axis, 1)
    left_top_in = shifted(left_top, axis, -1)
    low_half = pl.pallas_call(
        low_kernel,
        in_specs=[vmem] * 3,
        out_specs=[vmem] * 3,
        out_shape=[hold(low_hid), hold(low_part), hold(low_part)],
        cost_estimate=cost,
        compiler_params=grant,
        name="low",
    )
    both = held(both)
    low, far_low, right_low = low_half(normed, both, down)
    far_low_in = shifted(far_low, axis, -1)
    right_low_in = shifted(right_low, axis, 1)
    top, low = (held(top), held(low))
    rest = pl.pallas_call(
        rest_kernel,
        in_specs=[vmem] * 3,
        out_specs=[vmem] * 2,
        out_shape=[hold(part), hold(low_part)],
        cost_estimate=small,
        compiler_params=grant,
        name="rest",
    )
    right_top, left_low = rest(top, low, down)
    relay_top = relayed(far_top_in, right_top)
    relay_top_in = shifted(relay_top, axis, 1)
    relay_low = relayed(far_low_in, left_low)
    relay_low_in = shifted(relay_low, axis, -1)
    own = pl.pallas_call(
        own_kernel,
        in_specs=[vmem] * 4,
        out_specs=vmem,
        out_shape=hold((tok, owned), jnp.float32),
        cost_estimate=small,
        compiler_params=grant,
        name="own",
    )(top, low, down, base)
    return pl.pallas_call(
        settle_kernel,
        in_specs=[vmem] * 5,
        out_specs=vmem,
        out_shape=jax.ShapeDtypeStruct((tok, owned), jnp.bfloat16),
        cost_estimate=pl.CostEstimate(
            flops=2 * tok * owned, bytes_accessed=10 * tok * owned, transcendentals=0
        ),
        compiler_params=pltpu.CompilerParams(vmem_limit_bytes=12 << 20),
        name="close",
    )(held(own), left_top_in, relay_top_in, right_low_in, relay_low_in)


def rotate(values, positions):
    quarter = 16
    inverse = 10000.0 ** (-jnp.arange(quarter, dtype=jnp.float32) / quarter)

    def turn(part, place):
        angle = place.astype(jnp.float32)[:, None] * inverse[None, :]
        cosine = jnp.cos(angle)[:, None, :]
        sine = jnp.sin(angle)[:, None, :]
        first, second = (part[..., :quarter], part[..., quarter:])
        return jnp.concatenate(
            [first * cosine - second * sine, second * cosine + first * sine], axis=-1
        )

    grid_row = positions // GRID_W
    grid_col = positions % GRID_W
    return jnp.concatenate(
        [turn(values[..., :32], grid_row), turn(values[..., 32:], grid_col)], axis=-1
    )


def body(
    resid, queries, keys_values, sink, out_weight, norm_gain, gate_weight, up_weight, down_weight
):
    shard = jnp.concatenate((gate_weight, up_weight, down_weight.T), axis=1)
    weights = lax.all_gather(shard, "sp", axis=0, tiled=True)
    tok = queries.shape[0]
    heads_here = queries.shape[1] // HEAD_DIM
    kv_here = keys_values.shape[1]
    group = heads_here // kv_here
    offset = lax.axis_index("sp") * tok
    total_tokens = tok * lax.axis_size("sp")
    positions = offset + jnp.arange(tok, dtype=jnp.int32)
    rotated_q = rotate(
        queries.astype(jnp.float32).reshape(tok, heads_here, HEAD_DIM), positions
    ).astype(jnp.bfloat16)
    rotated_k = rotate(keys_values[..., :HEAD_DIM].astype(jnp.float32), positions).astype(
        jnp.bfloat16
    )
    joined = jnp.concatenate([rotated_k, keys_values[..., HEAD_DIM:]], axis=-1)
    padded = with_halo(joined, (("sp", 0),), WINDOW)
    blocks = tok // WINDOW
    key_blocks = jnp.stack(
        [padded[index * WINDOW : index * WINDOW + 3 * WINDOW] for index in range(blocks)]
    )
    grouped = rotated_q.reshape(blocks, WINDOW, kv_here, group, HEAD_DIM)
    scores = jnp.einsum(
        "nqkgd,njkd->nkgqj", grouped, key_blocks[..., :HEAD_DIM], preferred_element_type=jnp.float32
    ) * HEAD_DIM ** (-0.5)
    block_start = offset + WINDOW * jnp.arange(blocks, dtype=jnp.int32)
    query_pos = block_start[:, None] + jnp.arange(WINDOW, dtype=jnp.int32)[None, :]
    key_pos = block_start[:, None] - WINDOW + jnp.arange(3 * WINDOW, dtype=jnp.int32)[None, :]
    valid = (
        (jnp.abs(query_pos[:, :, None] - key_pos[:, None, :]) <= WINDOW)
        & (key_pos[:, None, :] >= 0)
        & (key_pos[:, None, :] < total_tokens)
    )
    scores = jnp.where(valid[:, None, None], scores, jnp.float32(-1e30))
    sink_grid = sink.reshape(kv_here, group)[None, :, :, None]
    top = jnp.maximum(jnp.max(scores, axis=-1), sink_grid)
    expo = jnp.exp(scores - top[..., None])
    denom = jnp.sum(expo, axis=-1) + jnp.exp(sink_grid - top)
    probs = (expo / denom[..., None]).astype(jnp.bfloat16)
    attended = jnp.einsum(
        "nkgqj,njkd->nqkgd", probs, key_blocks[..., HEAD_DIM:], preferred_element_type=jnp.float32
    )
    attended = attended.astype(jnp.bfloat16).reshape(tok, heads_here * HEAD_DIM)
    places = ring_places("tp")
    far, right, left, own = project(places, attended, out_weight, resid)
    stream = ring_sum(far, right, left, own, "tp")
    normed = normalised(places, norm_gain, stream, "tp")
    return feed_forward(places, normed, weights, stream, "tp")


def solution(mesh):
    return jax.shard_map(
        body,
        mesh=mesh,
        in_specs=(
            P(("grp", "sp"), "tp"),
            P(("grp", "sp"), "tp"),
            P(("grp", "sp"), "tp", None),
            P("tp"),
            P("tp", None),
            P(),
            P("sp", "tp"),
            P("sp", "tp"),
            P("tp", "sp"),
        ),
        out_specs=P(("grp", "sp"), "tp"),
        check_vma=False,
    )
```
